256 devices in a mesh: grp: 2 (over y), sp: 32 (over z, core), tp: 4 (over x).
Axes of the slice: x: 4, y: 2, z: 16, core: 2. Of those that a mesh axis runs over, the one named last changes fastest.
The devices are a block of a 4x16x16 slice.
Arguments:
- query_first: bfloat16 [12288, 512], P(('grp', 'sp'), 'tp'), parts along dimension 0, may hold values from -172 to 172
- key_first: bfloat16 [12288, 512], P(('grp', 'sp'), 'tp'), parts along dimension 0, may hold values from -7.8 to 7.8
- query_second: bfloat16 [12288, 1024], P(('grp', 'sp'), 'tp'), parts along dimension 0, may hold values from -172 to 172
- key_second: bfloat16 [12288, 1024], P(('grp', 'sp'), 'tp'), parts along dimension 0, may hold values from -7.8 to 7.8
- values: bfloat16 [12288, 2, 512], P(('grp', 'sp'), None, 'tp'), parts along dimension 0, may hold values from -6 to 6
- lambdas: float32 [2, 4], P(None, 'tp'), may hold values from 0.3 to 0.8
- residual: bfloat16 [12288, 2048], P(('grp', 'sp'), 'tp'), parts along dimension 0, may hold values from -130 to 130
- norm_gain: bfloat16 [2048], P('tp'), may hold values from 0.099609375 to 1.8984375
- out_weight: bfloat16 [2, 512, 2048], P(None, 'tp'), may hold values from -0.1875 to 0.1875
- gate_weight: bfloat16 [2048, 5632], P('sp', 'tp'), may hold values from -0.125 to 0.125
- up_weight: bfloat16 [2048, 5632], P('sp', 'tp'), may hold values from -0.125 to 0.125
- down_weight: bfloat16 [5632, 2048], P('tp', 'sp'), may hold values from -0.078125 to 0.078125
Outputs:
- layer_out: bfloat16 [12288, 2048], P(('grp', 'sp'), 'tp'), parts along dimension 0
The draws below stay inside these ranges and needn't reach their ends.
There are 2 independent parts, one for each index of `grp`. The reference program is written for one: setup_inputs(seed, part) draws one part's arguments, and reference() takes and returns one part's arrays. A program takes and returns all parts, laid end to end along the dimension named above; an argument that names none is the same for every part. Nothing has to cross between parts.
All inputs are finite; a program needn't handle non-finite values.
Results may differ from the reference program's by a relative error of at most 0.0065.
Values may be sent and summed in bfloat16 or wider, within the bound.
A program may use at most 128 MiB of HBM per device.

```python
import jax
import jax.numpy as jnp
from jax import lax

D = 2048
FF = 5632
HEADS = 4
DKA = 64
DKB = 128
DV = 128
SEQ = 6144


def paired_draw(key, salt, key_width):
    base = jax.random.fold_in(key, salt)
    key_draw = jax.random.normal(jax.random.fold_in(base, 1), (SEQ, HEADS * 2 * key_width), jnp.float32)
    query_draw = jax.random.normal(jax.random.fold_in(base, 2), (SEQ, HEADS * 2 * key_width), jnp.float32)
    keys_out = 1.3 * jnp.clip(key_draw, -6.0, 6.0)
    queries_out = 1.3 * jnp.clip(query_draw, -6.0, 6.0)
    return (queries_out, keys_out)


def draw_query_first(key, part):
    return paired_draw(key, 11, DKA)[0].astype(jnp.bfloat16)


def draw_key_first(key, part):
    return paired_draw(key, 11, DKA)[1].astype(jnp.bfloat16)


def draw_query_second(key, part):
    return paired_draw(key, 23, DKB)[0].astype(jnp.bfloat16)


def draw_key_second(key, part):
    return paired_draw(key, 23, DKB)[1].astype(jnp.bfloat16)


def draw_residual(key, part):
    base = jax.random.fold_in(key, 37)
    entries = jnp.clip(jax.random.normal(jax.random.fold_in(base, 1), (SEQ, D), jnp.float32), -6.0, 6.0)
    jitter = jnp.clip(jax.random.normal(jax.random.fold_in(base, 2), (1, D), jnp.float32), -2.0, 2.0)
    column = 0.3 * 10.0 ** (jnp.arange(D, dtype=jnp.float32)[None, :] / D + 0.1 * jitter)
    row_scale = 0.3 * 10.0 ** jax.random.uniform(jax.random.fold_in(base, 3), (SEQ, 1), jnp.float32)
    result = entries * column * row_scale
    return result.astype(jnp.bfloat16)


def block_scale(rng, dims, pieces, low, top_value):
    def one(axis_at, parts):
        heights = jax.random.uniform(jax.random.fold_in(jax.random.fold_in(rng, 6), axis_at), (parts,), jnp.float32, low / len(pieces), top_value / len(pieces))
        return jnp.repeat(jnp.exp(heights), dims[axis_at] // parts).reshape((-1,) + (1,) * (len(dims) - axis_at - 1))

    factor_of = one(*pieces[0])
    for cut in pieces[1:]:
        factor_of = factor_of * one(*cut)
    return factor_of


def bell_draw(rng, shape, spread, reach, pieces=(), held_as=jnp.bfloat16):
    values = jax.random.normal(rng, shape, jnp.float32) * spread
    if len(pieces) > 0:
        values = block_scale(rng, shape, pieces, -0.22, 0.18) * values
    return jnp.clip(values, min=-reach, max=reach).astype(held_as)


def setup_inputs(seed: int = 0, part: int = 0) -> dict:
    seeds = jax.random.split(jax.random.key(seed), 13)
    own_keys = jax.random.split(jax.random.fold_in(seeds[12], part), 13)
    query_first = draw_query_first(jax.random.fold_in(jax.random.fold_in(seeds[12], part), 71), part)
    key_first = draw_key_first(jax.random.fold_in(jax.random.fold_in(seeds[12], part), 71), part)
    query_second = draw_query_second(jax.random.fold_in(jax.random.fold_in(seeds[12], part), 71), part)
    key_second = draw_key_second(jax.random.fold_in(jax.random.fold_in(seeds[12], part), 71), part)
    values = bell_draw(own_keys[4], (SEQ, 2, HEADS * DV), 1.0, 6.0, ((0, 32), (2, 4)))
    lambdas = jnp.clip(0.3 + 0.5 * jax.random.uniform(seeds[5], (2, HEADS), jnp.float32) ** block_scale(seeds[5], (2, HEADS), ((1, 4),), -0.2, 0.2), 0.3, 0.8)
    residual = draw_residual(jax.random.fold_in(jax.random.fold_in(seeds[12], part), 71), part)
    norm_gain = jnp.clip(1.0 + 0.18 * jax.random.normal(seeds[7], (D,), jnp.float32), 0.099609375, 1.8984375).astype(jnp.bfloat16)
    out_weight = bell_draw(seeds[8], (2, HEADS * DV, D), (2 * HEADS * DV) ** -0.5, 0.1875, ((1, 4),))
    gate_weight = bell_draw(seeds[9], (D, FF), D ** -0.5, 0.125, ((0, 32), (1, 4)))
    up_weight = bell_draw(seeds[10], (D, FF), D ** -0.5, 0.125, ((0, 32), (1, 4)))
    down_weight = bell_draw(seeds[11], (FF, D), FF ** -0.5, 0.078125, ((0, 4), (1, 32)))
    return dict(query_first=query_first, key_first=key_first, query_second=query_second, key_second=key_second, values=values, lambdas=lambdas, residual=residual, norm_gain=norm_gain, out_weight=out_weight, gate_weight=gate_weight, up_weight=up_weight, down_weight=down_weight)


def one_head(query_rows, key_rows, value_rows, lam_value, key_width):
    block_rows = 512 if SEQ % 512 == 0 else SEQ
    blocks = SEQ // block_rows
    query_blocks = query_rows.reshape(blocks, block_rows, 2, key_width)
    starts = jnp.arange(blocks, dtype=jnp.int32) * block_rows
    key_pos = jnp.arange(SEQ, dtype=jnp.int32)[None, :]
    key_f32 = key_rows.astype(jnp.float32)
    value_f32 = value_rows.astype(jnp.float32)

    def per_block(inputs):
        query_block, offset = inputs
        query_pos = offset + jnp.arange(block_rows, dtype=jnp.int32)[:, None]
        allowed = key_pos <= query_pos
        scores = jnp.einsum('qmd,kmd->mqk', query_block.astype(jnp.float32), key_f32) * key_width ** (-0.5)
        scores = jnp.where(allowed, scores, -1e+30)
        peak = lax.optimization_barrier(jnp.max(scores, axis=-1, keepdims=True))
        weights = jnp.where(allowed, jnp.exp(scores - peak), 0.0)
        totals = lax.optimization_barrier(jnp.sum(weights, axis=-1, keepdims=True))
        rounded = weights.astype(jnp.bfloat16).astype(jnp.float32)
        map_out = jnp.einsum('mqk,ke->mqe', rounded, value_f32) / totals
        differ = map_out[0] - lam_value * map_out[1]
        scale = lax.rsqrt(lax.optimization_barrier(jnp.mean(differ * differ, axis=-1, keepdims=True)) + 1e-06)
        return (0.8 * differ * scale).astype(jnp.bfloat16)
    result = lax.map(per_block, (query_blocks, starts))
    return result.reshape(SEQ, DV)

def reference(query_first, key_first, query_second, key_second, values, lambdas, residual, norm_gain, out_weight, gate_weight, up_weight, down_weight):
    mixed = jnp.zeros((SEQ, D), jnp.float32)
    groups = ((query_first, key_first, DKA), (query_second, key_second, DKB))
    for group_idx in range(2):
        query_all, key_all, key_width = groups[group_idx]
        query_heads = query_all.reshape(SEQ, HEADS, 2, key_width)
        key_heads = key_all.reshape(SEQ, HEADS, 2, key_width)
        value_heads = values[:, group_idx].reshape(SEQ, HEADS, DV)
        outputs = []
        for head in range(HEADS):
            outputs.append(one_head(query_heads[:, head], key_heads[:, head], value_heads[:, head], lambdas[group_idx, head], key_width))
        attended = jnp.concatenate(outputs, axis=1)
        mixed = mixed + jnp.dot(attended, out_weight[group_idx], preferred_element_type=jnp.float32)
    stream = residual.astype(jnp.float32) + mixed
    scale = lax.rsqrt(lax.optimization_barrier(jnp.mean(stream * stream, axis=1, keepdims=True)) + 1e-06)
    normed = (stream * scale * norm_gain.astype(jnp.float32)).astype(jnp.bfloat16)
    gate = jnp.dot(normed, gate_weight, preferred_element_type=jnp.float32)
    up_part = jnp.dot(normed, up_weight, preferred_element_type=jnp.float32)
    hidden = (jax.nn.silu(gate) * up_part).astype(jnp.bfloat16)
    ffn = jnp.dot(hidden, down_weight, preferred_element_type=jnp.float32)
    return (stream + 0.5 * ffn).astype(jnp.bfloat16)
```

```python
import functools
import math

import jax
import jax.numpy as jnp
from jax import lax
from jax.experimental import pallas as pl
from jax.experimental.pallas import tpu as pltpu
from jax.sharding import PartitionSpec as P

MESH = pl.DeviceIdType.MESH
F32 = jnp.float32
BF16 = jnp.bfloat16
NT_DIMS = (((1,), (1,)), ((), ()))


class Ring:
    def __init__(self, index, buf, rows, start, size, across=None):
        self.index, self.buf, self.rows = index, buf, rows
        self.start, self.size, self.across = start, size, across


def kernel(
    nz, nt, lam_ref, q1_ref, q2_ref, gain_ref, kv_hbm, res_hbm, ow_hbm, gate_hbm, up_hbm, down_hbm,
    out_ref,
    kv, gate, up, down, ow, res, qa, qb, m_ref, l_ref, acc_ref, att, mix_send, mix_recv, mix_own,
    stream, sq, xg, hid, ffn_send, ffn_recv,
    zs, zr, ds, dr, ys, yr, es, er, xs, xr, local,
):
    g, s, t = lax.axis_index("grp"), lax.axis_index("sp"), lax.axis_index("tp")
    z, c = s // 2, s % 2
    half = nz // 2
    rows = res.shape[0]
    pair = 2 * rows
    feat = res.shape[1]
    wrows = gate_hbm.shape[0]
    part = g % 2
    sign = 1 - 2 * c

    def wrap(v):
        return lax.rem(v + 2 * nz, nz)

    def chip(v):
        return (g, 2 * wrap(v) + c, t)

    partner = (g, s + sign, t)
    across = (g + 1 - 2 * part, s, t)

    def other(k):
        return lax.rem(t + k, nt)

    own_kv = pl.ds(pl.multiple_of(rows * s, 16), rows)
    own_w = pl.ds(pl.multiple_of(wrows * s, 16), wrows)
    loads = [
        pltpu.make_async_copy(kv_hbm, kv.at[own_kv, :], local.at[0]),
        pltpu.make_async_copy(gate_hbm, gate.at[own_w, :], local.at[1]),
        pltpu.make_async_copy(up_hbm, up.at[own_w, :], local.at[2]),
        pltpu.make_async_copy(down_hbm, down.at[own_w, :], local.at[3]),
        pltpu.make_async_copy(ow_hbm, ow, local.at[4]),
        pltpu.make_async_copy(res_hbm, res, local.at[5]),
    ]
    for load in loads:
        load.start()
    barrier = pltpu.get_barrier_semaphore()
    peers = [chip(z + 1), chip(z - 1), partner, across] + [(g, s, other(k)) for k in range(1, nt)]
    for peer in peers:
        pl.semaphore_signal(barrier, inc=1, device_id=peer, device_id_type=MESH)

    w1, w2 = q1_ref.shape[1], q2_ref.shape[1]
    lane1 = lax.broadcasted_iota(jnp.int32, (rows, w1), 1)
    lane2 = lax.broadcasted_iota(jnp.int32, (rows, w2), 1)
    q1, q2 = q1_ref[...], q2_ref[...]
    qa[pl.ds(0, rows), :] = jnp.where(lane1 < w1 // 2, q1, jnp.zeros_like(q1))
    qa[pl.ds(rows, rows), :] = jnp.where(lane1 < w1 // 2, jnp.zeros_like(q1), q1)
    qb[pl.ds(0, rows), :] = jnp.where(lane2 < w2 // 2, q2, jnp.zeros_like(q2))
    qb[pl.ds(rows, rows), :] = jnp.where(lane2 < w2 // 2, jnp.zeros_like(q2), q2)

    pl.semaphore_wait(barrier, len(peers))

    def view(ring, slot, start=None, size=None):
        start = ring.start if start is None else start
        size = ring.size if size is None else size
        return ring.buf.at[pl.ds(pl.multiple_of(ring.rows * slot + start, 16), size), :]

    def remote(ref, send, recv, device):
        return pltpu.make_async_remote_copy(
            src_ref=ref, dst_ref=ref, send_sem=send, recv_sem=recv, device_id=device, device_id_type=MESH
        )

    def at_distance(way, d):
        return wrap(z - d) if way == 0 else wrap(z + d)

    def onward(ring, way, d):
        n = ring.index
        ref = view(ring, 2 * at_distance(way, d) + c)
        return remote(ref, zs.at[n, way, d], zr.at[n, way, d + 1], chip(z + 1 - 2 * way))

    def arrived(ring, way, d):
        n = ring.index
        ref = view(ring, 2 * at_distance(way, d) + c)
        return remote(ref, zs.at[n, way, d], zr.at[n, way, d], chip(z + 1 - 2 * way))

    def last_onward(ring):
        n = ring.index
        ref = view(ring, 2 * wrap(z - (half - 1) * sign) + c)
        return remote(ref, zs.at[n, 0, half - 1], zr.at[n, 0, half], chip(z + sign))

    def to_partner(ring, way, d):
        n = ring.index
        return remote(view(ring, 2 * at_distance(way, d) + c), ds.at[n, way, d], dr.at[n, way, d], partner)

    def from_partner(ring, way, d):
        n = ring.index
        ref = view(ring, 2 * at_distance(way, d) + 1 - c)
        return remote(ref, ds.at[n, way, d], dr.at[n, way, d], partner)

    def own_to_partner(ring, core):
        n = ring.index
        whole = ring.across is not None
        start, size = (0, ring.rows) if whole else (ring.start, ring.size)
        return remote(view(ring, 2 * z + core, start, size), ds.at[n, 0, 0], dr.at[n, 0, 0], partner)

    def to_across(ring, way, d):
        n = ring.across
        return remote(view(ring, 2 * at_distance(way, d) + c), ys.at[n, way, d], yr.at[n, way, d], across)

    def other_half(ring):
        return ring.size * (1 - part)

    def from_across(ring, way, d):
        n = ring.across
        ref = view(ring, 2 * at_distance(way, d) + c, other_half(ring))
        return remote(ref, ys.at[n, way, d], yr.at[n, way, d], across)

    def across_to_partner(ring, way, d, core):
        n = ring.across
        ref = view(ring, 2 * at_distance(way, d) + core, other_half(ring))
        return remote(ref, es.at[n, way, d], er.at[n, way, d], partner)

    def begin(rings):
        for ring in rings:
            for way in range(2):
                onward(ring, way, 0).start()
        for ring in rings:
            own_to_partner(ring, c).start()

    def landed(ring, way, d):
        arrived(ring, way, d).wait_recv()

    def pass_on(ring, way, d):
        to_partner(ring, way, d).start()
        if ring.across is not None:
            to_across(ring, way, d).start()

    def take_across(ring, way, d):
        from_across(ring, way, d).wait_recv()
        across_to_partner(ring, way, d, c).start()

    def turn(rings, then):
        def step(d, carry):
            for ring in rings:
                for way in range(2):
                    landed(ring, way, d)

                    @pl.when(d < half - 1)
                    def _():
                        onward(ring, way, d).start()

                    pass_on(ring, way, d)

                    if ring.across is not None:

                        @pl.when(d > 1)
                        def _():
                            take_across(ring, way, d - 1)

            @pl.when(d == half - 1)
            def _():
                for ring in rings:
                    last_onward(ring).start()

            then(d)
            return carry

        lax.fori_loop(1, half, step, 0)

    def turn_end(rings):
        for ring in rings:
            landed(ring, 0, half)
            pass_on(ring, 0, half)

    def finish_across(rings):
        for ring in rings:
            if ring.across is not None:
                for way in range(2):
                    take_across(ring, way, half - 1)
                take_across(ring, 0, half)

    def settle_partner(rings):
        for ring in rings:
            own_to_partner(ring, 1 - c).wait_recv()

            def step(d, carry):
                for way in range(2):
                    from_partner(ring, way, d).wait_recv()
                    if ring.across is not None:
                        across_to_partner(ring, way, d, 1 - c).wait_recv()
                return carry

            lax.fori_loop(1, half, step, 0)
            from_partner(ring, 0, half).wait_recv()
            if ring.across is not None:
                across_to_partner(ring, 0, half, 1 - c).wait_recv()

    def settle_sends(rings):
        for ring in rings:

            def step(d, carry):
                for way in range(2):
                    onward(ring, way, d - 1).wait_send()
                    to_partner(ring, way, d).wait_send()
                    if ring.across is not None:
                        to_across(ring, way, d).wait_send()
                        across_to_partner(ring, way, d, c).wait_send()
                return carry

            lax.fori_loop(1, half, step, 0)
            last_onward(ring).wait_send()
            own_to_partner(ring, c).wait_send()
            to_partner(ring, 0, half).wait_send()
            if ring.across is not None:
                to_across(ring, 0, half).wait_send()
                across_to_partner(ring, 0, half, c).wait_send()

    cut = rows // 2
    kv_rings = [Ring(0, kv, rows, 0, cut), Ring(1, kv, rows, cut, cut)]
    gate_ring = Ring(2, gate, wrows, 0, wrows)
    up_ring = Ring(3, up, wrows, (wrows // 2) * part, wrows // 2, across=0)
    down_ring = Ring(4, down, wrows, (wrows // 2) * part, wrows // 2, across=1)

    value_size = acc_ref.shape[2]
    log2e = 1.4426950408889634
    k_cols = ((0, w1), (w1, w2))
    v_at = w1 + w2

    def attend(zk, first):
        at = pl.ds(pl.multiple_of(pair * zk, 16), pair)
        for group in range(2):
            q_ref = (qa, qb)[group]
            col, width = k_cols[group]
            factor = (width // 2) ** (-0.5) * log2e
            scores = lax.dot_general(
                q_ref[...], kv[at, pl.ds(col, width)], NT_DIMS, preferred_element_type=F32
            )
            if first:
                q_at = lax.broadcasted_iota(jnp.int32, (pair, pair), 0)
                k_at = lax.broadcasted_iota(jnp.int32, (pair, pair), 1)
                q_at = jnp.where(q_at >= rows, q_at - rows, q_at) + rows * c
                scores = jnp.where(k_at <= q_at, scores, -1e30)
            peak = jnp.max(scores, axis=1, keepdims=True)
            if not first:
                old = m_ref[group][:, :1]
                peak = jnp.maximum(old, peak)
                alpha = jnp.exp2((old - peak) * factor)
            weights = jnp.exp2((scores - peak) * factor)
            total = jnp.sum(weights, axis=1, keepdims=True)
            values = kv[at, pl.ds(v_at + group * value_size, value_size)]
            out = jnp.dot(weights.astype(BF16), values, preferred_element_type=F32)
            if not first:
                total = total + alpha * l_ref[group][:, :1]
                out = out + alpha * acc_ref[group]
            m_ref[group] = jnp.broadcast_to(peak, (pair, 128))
            l_ref[group] = jnp.broadcast_to(total, (pair, 128))
            acc_ref[group] = out

    def attend_step(d):
        def one(i, carry):
            zk = jnp.where(i == 0, z - d, z + d - nz)

            @pl.when(zk >= 0)
            def _():
                attend(zk, False)

            return carry

        lax.fori_loop(0, 2, one, 0)

    def swap(ref_from, ref_to, which, k):
        return pltpu.make_async_remote_copy(
            src_ref=ref_from, dst_ref=ref_to, send_sem=xs.at[which, k - 1], recv_sem=xr.at[which, k - 1],
            device_id=(g, s, other(k)), device_id_type=MESH,
        )

    def mine(which, k):
        if which == 0:
            return swap(mix_send.at[k - 1], mix_recv.at[k - 1], 0, k)
        if which == 1:
            cols = xg.at[:, pl.ds(pl.multiple_of(feat * t, 128), feat)]
            return swap(cols, cols, 1, k)
        if which == 2:
            return swap(sq.at[t], sq.at[t], 2, k)
        return swap(ffn_send.at[k - 1], ffn_recv.at[k - 1], 3, k)

    def theirs(which, k):
        frm = lax.rem(t + nt - k, nt)
        if which == 1:
            cols = xg.at[:, pl.ds(pl.multiple_of(feat * frm, 128), feat)]
            return swap(cols, cols, 1, k)
        if which == 2:
            return swap(sq.at[frm], sq.at[frm], 2, k)
        return mine(which, k)

    loads[0].wait()
    begin(kv_rings)
    for load in loads[1:4]:
        load.wait()
    ffn_rings = [gate_ring, up_ring]

    def kv_then(d):
        @pl.when(d == 1)
        def _():
            for ring in kv_rings:
                own_to_partner(ring, 1 - c).wait_recv()
            attend(z, True)

        @pl.when(d == half - 2)
        def _():
            begin(ffn_rings)

        @pl.when(d > 1)
        def _():
            for ring in kv_rings:
                for way in range(2):
                    from_partner(ring, way, d - 1).wait_recv()
            attend_step(d - 1)

    turn(kv_rings, kv_then)
    turn_end(kv_rings)
    for ring in kv_rings:
        for way in range(2):
            from_partner(ring, way, half - 1).wait_recv()
    attend_step(half - 1)
    for ring in kv_rings:
        from_partner(ring, 0, half).wait_recv()

    @pl.when(z >= half)
    def _():
        attend(z - half, False)

    for group in range(2):
        map_out = acc_ref[group] / l_ref[group]
        differ = map_out[:rows] - lam_ref[group, 0] * map_out[rows:]
        scale = lax.rsqrt(jnp.mean(differ * differ, axis=1, keepdims=True) + 1e-06)
        att[:, pl.ds(group * value_size, value_size)] = (0.8 * differ * scale).astype(BF16)
    loads[4].wait()
    for k in range(1, nt):
        cols = pl.ds(pl.multiple_of(feat * other(k), 128), feat)
        mix_send[k - 1] = jnp.dot(att[...], ow[:, cols], preferred_element_type=F32).astype(BF16)
    mix_own[...] = jnp.dot(
        att[...], ow[:, pl.ds(pl.multiple_of(feat * t, 128), feat)], preferred_element_type=F32
    )
    for k in range(1, nt):
        mine(0, k).start()
    loads[5].wait()

    def ffn_then(d):
        @pl.when(d == 3)
        def _():
            total = mix_own[...] + res[...].astype(F32)
            for k in range(1, nt):
                theirs(0, k).wait_recv()
                total = total + mix_recv[k - 1].astype(F32)
            stream[...] = total
            sq[t] = jnp.broadcast_to(jnp.sum(total * total, axis=1, keepdims=True), sq.shape[1:])
            xg[:, pl.ds(pl.multiple_of(feat * t, 128), feat)] = (
                total * gain_ref[...].astype(F32)
            ).astype(BF16)

        @pl.when(d == 4)
        def _():
            for k in range(1, nt):
                mine(1, k).start()
                mine(2, k).start()

        @pl.when(d == half - 2)
        def _():
            begin([down_ring])

    turn(ffn_rings, ffn_then)
    turn_end(ffn_rings)
    finish_across(ffn_rings)
    settle_partner(ffn_rings)
    for k in range(1, nt):
        theirs(1, k).wait_recv()
        theirs(2, k).wait_recv()
    squares = sq[0]
    for k in range(1, nt):
        squares = squares + sq[k]
    model = feat * nt
    row_scale = lax.rsqrt(squares / model + 1e-06)[:, :1]
    m_ref[0, pl.ds(0, rows), :] = jnp.broadcast_to(row_scale, (rows, 128))

    hidden = hid.shape[1]
    tile = 256

    def hidden_tile(cols):
        scale = m_ref[0, pl.ds(0, rows), :][:, :1]
        gates = jnp.dot(xg[...], gate[:, cols], preferred_element_type=F32) * scale
        ups = jnp.dot(xg[...], up[:, cols], preferred_element_type=F32) * scale
        hid[:, cols] = (gates / (1.0 + jnp.exp(-gates)) * ups).astype(BF16)

    tiles, rest = hidden // tile, hidden % tile

    def down_then(d):
        @pl.when(d <= tiles)
        def _():
            hidden_tile(pl.ds(pl.multiple_of((d - 1) * tile, 128), tile))

        @pl.when(d == tiles + 1)
        def _():
            hidden_tile(pl.ds(tiles * tile, rest))

    turn([down_ring], down_then)
    turn_end([down_ring])
    finish_across([down_ring])
    settle_partner([down_ring])

    def share(owner):
        parts = []
        for i in range(2):
            at = pl.ds(pl.multiple_of(feat * owner + i * (feat // 2), 16), feat // 2)
            parts.append(lax.dot_general(hid[...], down[at, :], NT_DIMS, preferred_element_type=F32))
        return jnp.concatenate(parts, axis=1)

    for k in (2, 1, 3):
        ffn_send[k - 1] = share(other(k)).astype(BF16)
    own = share(t)
    for k in (2, 1, 3):
        mine(3, k).start()
    settle_sends(kv_rings + ffn_rings + [down_ring])
    for which in range(3):
        for k in range(1, nt):
            mine(which, k).wait_send()
    for k in range(1, nt):
        theirs(3, k).wait_recv()
        own = own + ffn_recv[k - 1].astype(F32)
    out_ref[...] = (stream[...] + 0.5 * own).astype(BF16)
    for k in range(1, nt):
        mine(3, k).wait_send()


def layer(
    nz, nt, query_first, key_first, query_second, key_second, values, lambdas, residual, norm_gain,
    out_weight, gate_weight, up_weight, down_weight,
):
    rows, feat = residual.shape
    wrows, hidden = gate_weight.shape
    value_size = values.shape[2]
    model = feat * nt
    kv = jnp.concatenate([key_first, key_second, values.reshape(rows, -1)], axis=1)
    w1, w2 = query_first.shape[1], query_second.shape[1]
    any_ref = pl.BlockSpec(memory_space=pltpu.HBM)
    vmem = pl.BlockSpec(memory_space=pltpu.VMEM)
    half = nz // 2
    dma = pltpu.SemaphoreType.DMA
    return pl.pallas_call(
        functools.partial(kernel, nz, nt),
        out_shape=jax.ShapeDtypeStruct((rows, feat), BF16),
        in_specs=[pl.BlockSpec(memory_space=pltpu.SMEM), vmem, vmem, vmem] + [any_ref] * 6,
        out_specs=vmem,
        scratch_shapes=[
            pltpu.VMEM((2 * nz * rows, kv.shape[1]), BF16),
            pltpu.VMEM((2 * nz * wrows, hidden), BF16),
            pltpu.VMEM((2 * nz * wrows, hidden), BF16),
            pltpu.VMEM((2 * nz * wrows, hidden), BF16),
            pltpu.VMEM((2 * value_size, model), BF16),
            pltpu.VMEM((rows, feat), BF16),
            pltpu.VMEM((2 * rows, w1), BF16),
            pltpu.VMEM((2 * rows, w2), BF16),
            pltpu.VMEM((2, 2 * rows, 128), F32),
            pltpu.VMEM((2, 2 * rows, 128), F32),
            pltpu.VMEM((2, 2 * rows, value_size), F32),
            pltpu.VMEM((rows, 2 * value_size), BF16),
            pltpu.VMEM((nt - 1, rows, feat), BF16),
            pltpu.VMEM((nt - 1, rows, feat), BF16),
            pltpu.VMEM((rows, feat), F32),
            pltpu.VMEM((rows, feat), F32),
            pltpu.VMEM((nt, rows, 128), F32),
            pltpu.VMEM((rows, model), BF16),
            pltpu.VMEM((rows, hidden), BF16),
            pltpu.VMEM((nt - 1, rows, feat), BF16),
            pltpu.VMEM((nt - 1, rows, feat), BF16),
            dma((5, 2, half + 1)),
            dma((5, 2, half + 1)),
            dma((5, 2, half + 1)),
            dma((5, 2, half + 1)),
            dma((2, 2, half + 1)),
            dma((2, 2, half + 1)),
            dma((2, 2, half + 1)),
            dma((2, 2, half + 1)),
            dma((4, nt - 1)),
            dma((4, nt - 1)),
            dma((6,)),
        ],
        compiler_params=pltpu.CompilerParams(
            collective_id=0, has_side_effects=True, vmem_limit_bytes=60 * 2**20
        ),
    )(
        lambdas, query_first, query_second, norm_gain.reshape(1, feat), kv, residual,
        out_weight.reshape(2 * value_size, model), gate_weight, up_weight, down_weight.T,
    )


def solution(mesh):
    return jax.shard_map(
        functools.partial(layer, mesh.shape["sp"] // 2, mesh.shape["tp"]),
        mesh=mesh,
        in_specs=(
            P(("grp", "sp"), "tp"),
            P(("grp", "sp"), "tp"),
            P(("grp", "sp"), "tp"),
            P(("grp", "sp"), "tp"),
            P(("grp", "sp"), None, "tp"),
            P(None, "tp"),
            P(("grp", "sp"), "tp"),
            P("tp"),
            P(None, "tp", None),
            P("sp", "tp"),
            P("sp", "tp"),
            P("tp", "sp"),
        ),
        out_specs=P(("grp", "sp"), "tp"),
        check_vma=False,
    )
```

```python
import functools
import math

import jax
import jax.numpy as jnp
from jax import lax
from jax.experimental import pallas as pl
from jax.experimental.pallas import tpu as pltpu
from jax.sharding import PartitionSpec as P

MESH = pl.DeviceIdType.MESH
F32 = jnp.float32
BF16 = jnp.bfloat16
NT_DIMS = (((1,), (1,)), ((), ()))
SPLIT = 16


class Ring:
    def __init__(self, index, buf, rows, low, size, across=None):
        self.index, self.buf, self.rows = index, buf, rows
        self.low, self.size, self.across = low, size, across


def kernel(
    nz, nt, lam_ref, q1_ref, q2_ref, gain_ref, k1_hbm, k2_hbm, v_hbm, res_hbm, ow_hbm, gate_hbm, up_hbm, down_hbm,
    out_ref,
    kv, gate, up, down, ow, res, qa, qb, m_ref, l_ref, acc_ref, att, mix_send, mix_recv, mix_own,
    stream, sq, xg, hid, ffn_send, ffn_recv, ffn_own,
    sent, zr, dr, yr, er, xs, xr, local,
):
    g, s, t = lax.axis_index("grp"), lax.axis_index("sp"), lax.axis_index("tp")
    z, c = s // 2, s % 2
    half = nz // 2
    rows = res.shape[0]
    pair = 2 * rows
    feat = res.shape[1]
    wrows = gate_hbm.shape[0]
    part = g % 2
    sign = 1 - 2 * c

    def wrap(v):
        return lax.rem(v + 2 * nz, nz)

    def chip(v):
        return (g, 2 * wrap(v) + c, t)

    partner = (g, s + sign, t)
    across = (g + 1 - 2 * part, s, t)

    def other(k):
        return lax.rem(t + k, nt)

    own_kv = pl.ds(pl.multiple_of(rows * s, 16), rows)
    own_w = pl.ds(pl.multiple_of(wrows * s, 16), wrows)
    k1_width, k2_width, v_width = k1_hbm.shape[1], k2_hbm.shape[1], v_hbm.shape[1]
    loads = [
        pltpu.make_async_copy(k1_hbm, kv.at[own_kv, pl.ds(0, k1_width)], local.at[0]),
        pltpu.make_async_copy(k2_hbm, kv.at[own_kv, pl.ds(k1_width, k2_width)], local.at[1]),
        pltpu.make_async_copy(v_hbm, kv.at[own_kv, pl.ds(k1_width + k2_width, v_width)], local.at[2]),
        pltpu.make_async_copy(up_hbm, up.at[own_w, :], local.at[3]),
        pltpu.make_async_copy(gate_hbm, gate.at[own_w, :], local.at[4]),
        pltpu.make_async_copy(down_hbm, down.at[own_w, :], local.at[5]),
        pltpu.make_async_copy(ow_hbm, ow, local.at[6]),
        pltpu.make_async_copy(res_hbm, res, local.at[7]),
    ]
    for load in loads:
        load.start()
    barrier = pltpu.get_barrier_semaphore()
    peers = [chip(z + 1), chip(z - 1), partner, across] + [(g, s, other(k)) for k in range(1, nt)]
    for peer in peers:
        pl.semaphore_signal(barrier, inc=1, device_id=peer, device_id_type=MESH)

    w1, w2 = q1_ref.shape[1], q2_ref.shape[1]
    lane1 = lax.broadcasted_iota(jnp.int32, (rows, w1), 1)
    lane2 = lax.broadcasted_iota(jnp.int32, (rows, w2), 1)
    q1, q2 = q1_ref[...], q2_ref[...]
    qa[pl.ds(0, rows), :] = jnp.where(lane1 < w1 // 2, q1, jnp.zeros_like(q1))
    qa[pl.ds(rows, rows), :] = jnp.where(lane1 < w1 // 2, jnp.zeros_like(q1), q1)
    qb[pl.ds(0, rows), :] = jnp.where(lane2 < w2 // 2, q2, jnp.zeros_like(q2))
    qb[pl.ds(rows, rows), :] = jnp.where(lane2 < w2 // 2, jnp.zeros_like(q2), q2)

    pl.semaphore_wait(barrier, len(peers))

    def view(ring, slot, start, size):
        return ring.buf.at[pl.ds(pl.multiple_of(ring.rows * slot + start, 8), size), :]

    def of_mine(ring, slot):
        shift = 0 if ring.across is None else ring.size * part
        return view(ring, slot, ring.low + shift, ring.size)

    def of_across(ring, slot):
        return view(ring, slot, ring.low + ring.size * (1 - part), ring.size)

    def remote(ring, ref, recv, device):
        return pltpu.make_async_remote_copy(
            src_ref=ref, dst_ref=ref, send_sem=sent.at[ring.index], recv_sem=recv,
            device_id=device, device_id_type=MESH,
        )

    def total(ring, count, recv):
        return remote(ring, ring.buf.at[pl.ds(0, count * ring.size), :], recv, partner)

    def at_distance(way, d):
        return 2 * (wrap(z - d) if way == 0 else wrap(z + d))

    def onward(ring, way, d):
        ref = of_mine(ring, at_distance(way, d) + c)
        return remote(ring, ref, zr.at[ring.index, way, d + 1], chip(z + 1 - 2 * way))

    def landed(ring, way, d):
        ref = of_mine(ring, at_distance(way, d) + c)
        remote(ring, ref, zr.at[ring.index, way, d], partner).wait_recv()

    def last_onward(ring):
        ref = of_mine(ring, 2 * wrap(z - (half - 1) * sign) + c)
        return remote(ring, ref, zr.at[ring.index, 0, half], chip(z + sign))

    def begin(rings):
        for ring in rings:
            for way in range(2):
                onward(ring, way, 0).start()
        for ring in rings:
            size = ring.size if ring.across is None else 2 * ring.size
            ref = view(ring, 2 * z + c, ring.low, size)
            remote(ring, ref, dr.at[ring.index, 0], partner).start()

    def pass_on(ring, way, d):
        ref = of_mine(ring, at_distance(way, d) + c)
        if ring.across is not None:
            remote(ring, ref, yr.at[ring.across, way, d], across).start()
        remote(ring, ref, dr.at[ring.index, d], partner).start()

    def take_across(ring, way, d):
        ref = of_across(ring, at_distance(way, d) + c)
        remote(ring, ref, yr.at[ring.across, way, d], across).wait_recv()
        remote(ring, ref, er.at[ring.across, d], partner).start()

    def from_partner(ring, d, count):
        if ring.across is not None:
            total(ring, 2 if count == 0 else count, dr.at[ring.index, d]).wait_recv()
            if count > 0:
                total(ring, count, er.at[ring.across, d]).wait_recv()
        else:
            total(ring, 1 if count == 0 else count, dr.at[ring.index, d]).wait_recv()

    def all_from_partner(rings):
        for ring in rings:
            from_partner(ring, 0, 0)

            def step(d, carry):
                from_partner(ring, d, 2)
                return carry

            lax.fori_loop(1, half, step, 0)
            from_partner(ring, half, 1)

    def turn(rings, then):
        def step(d, carry):
            for ring in rings:
                for way in range(2):
                    landed(ring, way, d)

                    @pl.when(d < half - 1)
                    def _():
                        onward(ring, way, d).start()

                    pass_on(ring, way, d)

                    if ring.across is not None:

                        @pl.when(d > 1)
                        def _():
                            take_across(ring, way, d - 1)

            @pl.when(d == half - 1)
            def _():
                for ring in rings:
                    last_onward(ring).start()

            then(d)
            return carry

        lax.fori_loop(1, half, step, 0)

    def turn_end(rings):
        for ring in rings:
            landed(ring, 0, half)
            pass_on(ring, 0, half)

    def finish_across(rings):
        for ring in rings:
            if ring.across is not None:
                for way in range(2):
                    take_across(ring, way, half - 1)
                take_across(ring, 0, half)

    def all_sent(rings):
        for ring in rings:
            count = 4 * half - 1 if ring.across is None else 8 * half - 2
            total(ring, count, dr.at[ring.index, 0]).wait_send()

    cut = rows // 2
    kv_rings = [Ring(0, kv, rows, 0, cut), Ring(1, kv, rows, cut, cut)]
    up_rings = [Ring(2, up, wrows, 0, wrows // 2, across=0)]
    gate_rings = [
        Ring(3, gate, wrows, 0, SPLIT, across=1), Ring(4, gate, wrows, 2 * SPLIT, wrows - 2 * SPLIT)
    ]
    down_rings = [
        Ring(5, down, wrows, 0, SPLIT, across=2), Ring(6, down, wrows, 2 * SPLIT, wrows - 2 * SPLIT)
    ]

    value_size = acc_ref.shape[2]
    log2e = 1.4426950408889634
    k_cols = ((0, w1), (w1, w2))
    v_at = w1 + w2

    def attend(zk, first):
        at = pl.ds(pl.multiple_of(pair * zk, 16), pair)
        for group in range(2):
            q_ref = (qa, qb)[group]
            col, width = k_cols[group]
            factor = (width // 2) ** (-0.5) * log2e
            scores = lax.dot_general(
                q_ref[...], kv[at, pl.ds(col, width)], NT_DIMS, preferred_element_type=F32
            )
            if first:
                q_at = lax.broadcasted_iota(jnp.int32, (pair, pair), 0)
                k_at = lax.broadcasted_iota(jnp.int32, (pair, pair), 1)
                q_at = jnp.where(q_at >= rows, q_at - rows, q_at) + rows * c
                scores = jnp.where(k_at <= q_at, scores, -1e30)
            peak = jnp.max(scores, axis=1, keepdims=True)
            if not first:
                old = m_ref[group][:, :1]
                peak = jnp.maximum(old, peak)
                alpha = jnp.exp2((old - peak) * factor)
            weights = jnp.exp2((scores - peak) * factor)
            total = jnp.sum(weights, axis=1, keepdims=True)
            values = kv[at, pl.ds(v_at + group * value_size, value_size)]
            out = jnp.dot(weights.astype(BF16), values, preferred_element_type=F32)
            if not first:
                total = total + alpha * l_ref[group][:, :1]
                out = out + alpha * acc_ref[group]
            m_ref[group] = jnp.broadcast_to(peak, (pair, 128))
            l_ref[group] = jnp.broadcast_to(total, (pair, 128))
            acc_ref[group] = out

    def attend_step(d):
        def one(i, carry):
            zk = jnp.where(i == 0, z - d, z + d - nz)

            @pl.when(zk >= 0)
            def _():
                attend(zk, False)

            return carry

        lax.fori_loop(0, 2, one, 0)

    def swap(ref_from, ref_to, which, k):
        return pltpu.make_async_remote_copy(
            src_ref=ref_from, dst_ref=ref_to, send_sem=xs.at[which, k - 1], recv_sem=xr.at[which, k - 1],
            device_id=(g, s, other(k)), device_id_type=MESH,
        )

    def mine(which, k):
        if which == 0:
            return swap(mix_send.at[k - 1], mix_recv.at[k - 1], 0, k)
        if which == 1:
            cols = xg.at[:, pl.ds(pl.multiple_of(feat * t, 128), feat)]
            return swap(cols, cols, 1, k)
        if which == 2:
            return swap(sq.at[t], sq.at[t], 2, k)
        return swap(ffn_send.at[k - 1], ffn_recv.at[k - 1], 3, k)

    def theirs(which, k):
        frm = lax.rem(t + nt - k, nt)
        if which == 1:
            cols = xg.at[:, pl.ds(pl.multiple_of(feat * frm, 128), feat)]
            return swap(cols, cols, 1, k)
        if which == 2:
            return swap(sq.at[frm], sq.at[frm], 2, k)
        return mine(which, k)

    for load in loads[:3]:
        load.wait()
    begin(kv_rings)
    loads[3].wait()
    begin(up_rings)
    for load in loads[4:6]:
        load.wait()

    def kv_then(d):
        @pl.when(d == 1)
        def _():
            for ring in kv_rings:
                from_partner(ring, 0, 0)
            attend(z, True)

        @pl.when(d == half - 2)
        def _():
            begin(gate_rings)

        @pl.when(d > 1)
        def _():
            for ring in kv_rings:
                from_partner(ring, d - 1, 2)
            attend_step(d - 1)

    turn(kv_rings + up_rings, kv_then)
    turn_end(kv_rings + up_rings)
    for ring in kv_rings:
        from_partner(ring, half - 1, 2)
    attend_step(half - 1)
    for ring in kv_rings:
        from_partner(ring, half, 1)

    @pl.when(z >= half)
    def _():
        attend(z - half, False)

    for group in range(2):
        map_out = acc_ref[group] / l_ref[group]
        differ = map_out[:rows] - lam_ref[0, group] * map_out[rows:]
        scale = lax.rsqrt(jnp.mean(differ * differ, axis=1, keepdims=True) + 1e-06)
        att[:, pl.ds(group * value_size, value_size)] = (0.8 * differ * scale).astype(BF16)
    loads[6].wait()
    order = (2, 1, 3)
    for k in order:
        cols = pl.ds(pl.multiple_of(feat * other(k), 128), feat)
        mix_send[k - 1] = jnp.dot(att[...], ow[:, cols], preferred_element_type=F32).astype(BF16)
    mix_own[...] = jnp.dot(
        att[...], ow[:, pl.ds(pl.multiple_of(feat * t, 128), feat)], preferred_element_type=F32
    )
    for k in order:
        mine(0, k).start()
    loads[7].wait()

    def gate_then(d):
        @pl.when(d == 4)
        def _():
            acc = mix_own[...] + res[...].astype(F32)
            for k in order:
                theirs(0, k).wait_recv()
                acc = acc + mix_recv[k - 1].astype(F32)
            stream[...] = acc
            sq[t] = jnp.broadcast_to(jnp.sum(acc * acc, axis=1, keepdims=True), sq.shape[1:])
            xg[:, pl.ds(pl.multiple_of(feat * t, 128), feat)] = (
                acc * gain_ref[...].astype(F32)
            ).astype(BF16)
            for k in order:
                mine(1, k).start()
                mine(2, k).start()

        @pl.when(d == half - 2)
        def _():
            begin(down_rings)

    finish_across(up_rings)
    turn(gate_rings, gate_then)
    turn_end(gate_rings)
    all_from_partner(up_rings)

    hidden = hid.shape[1]
    tile = 256

    def hidden_tile(cols):
        scale = m_ref[0, pl.ds(0, rows), :][:, :1]
        gates = jnp.dot(xg[...], gate[:, cols], preferred_element_type=F32) * scale
        ups = jnp.dot(xg[...], up[:, cols], preferred_element_type=F32) * scale
        hid[:, cols] = (gates / (1.0 + jnp.exp(-gates)) * ups).astype(BF16)

    tiles, rest = hidden // tile, hidden % tile

    def hidden_units():
        finish_across(gate_rings)
        all_from_partner(gate_rings)
        for k in order:
            theirs(1, k).wait_recv()
            theirs(2, k).wait_recv()
        squares = sq[0]
        for k in range(1, nt):
            squares = squares + sq[k]
        m_ref[0, pl.ds(0, rows), :] = lax.rsqrt(squares / (feat * nt) + 1e-06)

        def one(i, carry):
            hidden_tile(pl.ds(pl.multiple_of(i * tile, 128), tile))
            return carry

        lax.fori_loop(0, tiles, one, 0)
        hidden_tile(pl.ds(tiles * tile, rest))

    def share(owner):
        parts = []
        for i in range(2):
            at = pl.ds(pl.multiple_of(feat * owner + i * (feat // 2), 16), feat // 2)
            parts.append(lax.dot_general(hid[...], down[at, :], NT_DIMS, preferred_element_type=F32))
        return jnp.concatenate(parts, axis=1)

    def give(owner):
        value = share(owner)
        k = lax.rem(owner - t + nt, nt)

        @pl.when(k == 0)
        def _():
            ffn_own[...] = value

        @pl.when(k > 0)
        def _():
            ffn_send[k - 1] = value.astype(BF16)
            mine(3, k).start()

    chips = nz // nt
    here, place = z // chips, lax.rem(z, chips)

    def near(v):
        return lax.rem(here + v + nt, nt)

    def down_then(d):
        @pl.when(d == 1)
        def _():
            for ring in down_rings:
                from_partner(ring, 0, 0)

        @pl.when(d > 1)
        def _():
            for ring in down_rings:
                from_partner(ring, d - 1, 2)

        @pl.when(d == 2)
        def _():
            hidden_units()

        ready = (d == chips) | (d == chips + 1 + place) | (d == 2 * chips - place)

        @pl.when(ready)
        def _():
            give(jnp.where(d == chips, here, jnp.where(d == chips + 1 + place, near(-1), near(1))))

    turn(down_rings, down_then)
    turn_end(down_rings)
    finish_across(down_rings)
    for ring in down_rings:
        from_partner(ring, half - 1, 2)

    @pl.when((place == 0) | (place == chips - 1))
    def _():
        give(jnp.where(place == 0, near(1), near(-1)))

    for ring in down_rings:
        from_partner(ring, half, 1)
    give(near(2))
    all_sent(kv_rings + up_rings + gate_rings + down_rings)
    for which in range(3):
        for k in range(1, nt):
            mine(which, k).wait_send()
    acc = ffn_own[...]
    for k in range(1, nt):
        theirs(3, k).wait_recv()
        acc = acc + ffn_recv[k - 1].astype(F32)
    out_ref[...] = (stream[...] + 0.5 * acc).astype(BF16)
    for k in range(1, nt):
        mine(3, k).wait_send()


def layer(
    nz, nt, query_first, key_first, query_second, key_second, values, lambdas, residual, norm_gain,
    out_weight, gate_weight, up_weight, down_weight,
):
    rows, feat = residual.shape
    wrows, hidden = gate_weight.shape
    value_size = values.shape[2]
    model = feat * nt
    kv_width = key_first.shape[1] + key_second.shape[1] + 2 * value_size
    w1, w2 = query_first.shape[1], query_second.shape[1]
    any_ref = pl.BlockSpec(memory_space=pltpu.HBM)
    vmem = pl.BlockSpec(memory_space=pltpu.VMEM)
    half = nz // 2
    dma = pltpu.SemaphoreType.DMA
    return pl.pallas_call(
        functools.partial(kernel, nz, nt),
        out_shape=jax.ShapeDtypeStruct((rows, feat), BF16),
        in_specs=[pl.BlockSpec(memory_space=pltpu.SMEM), vmem, vmem, vmem] + [any_ref] * 8,
        out_specs=vmem,
        scratch_shapes=[
            pltpu.VMEM((2 * nz * rows, kv_width), BF16),
            pltpu.VMEM((2 * nz * wrows, hidden), BF16),
            pltpu.VMEM((2 * nz * wrows, hidden), BF16),
            pltpu.VMEM((2 * nz * wrows, hidden), BF16),
            pltpu.VMEM((2 * value_size, model), BF16),
            pltpu.VMEM((rows, feat), BF16),
            pltpu.VMEM((2 * rows, w1), BF16),
            pltpu.VMEM((2 * rows, w2), BF16),
            pltpu.VMEM((2, 2 * rows, 128), F32),
            pltpu.VMEM((2, 2 * rows, 128), F32),
            pltpu.VMEM((2, 2 * rows, value_size), F32),
            pltpu.VMEM((rows, 2 * value_size), BF16),
            pltpu.VMEM((nt - 1, rows, feat), BF16),
            pltpu.VMEM((nt - 1, rows, feat), BF16),
            pltpu.VMEM((rows, feat), F32),
            pltpu.VMEM((rows, feat), F32),
            pltpu.VMEM((nt, rows, 128), F32),
            pltpu.VMEM((rows, model), BF16),
            pltpu.VMEM((rows, hidden), BF16),
            pltpu.VMEM((nt - 1, rows, feat), BF16),
            pltpu.VMEM((nt - 1, rows, feat), BF16),
            pltpu.VMEM((rows, feat), F32),
            dma((7,)),
            dma((7, 2, half + 1)),
            dma((7, half + 1)),
            dma((3, 2, half + 1)),
            dma((3, half + 1)),
            dma((4, nt - 1)),
            dma((4, nt - 1)),
            dma((8,)),
        ],
        compiler_params=pltpu.CompilerParams(
            collective_id=0, has_side_effects=True, vmem_limit_bytes=60 * 2**20
        ),
    )(
        lambdas.T, query_first, query_second, norm_gain.reshape(1, feat), key_first, key_second,
        values.reshape(rows, -1), residual,
        out_weight.reshape(2 * value_size, model), gate_weight, up_weight, down_weight.T,
    )


def solution(mesh):
    return jax.shard_map(
        functools.partial(layer, mesh.shape["sp"] // 2, mesh.shape["tp"]),
        mesh=mesh,
        in_specs=(
            P(("grp", "sp"), "tp"),
            P(("grp", "sp"), "tp"),
            P(("grp", "sp"), "tp"),
            P(("grp", "sp"), "tp"),
            P(("grp", "sp"), None, "tp"),
            P(None, "tp"),
            P(("grp", "sp"), "tp"),
            P("tp"),
            P(None, "tp", None),
            P("sp", "tp"),
            P("sp", "tp"),
            P("tp", "sp"),
        ),
        out_specs=P(("grp", "sp"), "tp"),
        check_vma=False,
    )
```

```python
import functools
import math

import jax
import jax.numpy as jnp
from jax import lax
from jax.experimental import pallas as pl
from jax.experimental.pallas import tpu as pltpu
from jax.sharding import PartitionSpec as P

MESH = pl.DeviceIdType.MESH
F32 = jnp.float32
BF16 = jnp.bfloat16
NT_DIMS = (((1,), (1,)), ((), ()))
SPLIT = 16
GATE_AT, DOWN_AT = 7, 9
STREAM_AT, HIDDEN_AT = 12, 16
ORDER = (2, 1, 3)


class Ring:
    def __init__(self, index, buf, rows, low, size, across=None):
        self.index, self.buf, self.rows = index, buf, rows
        self.low, self.size, self.across = low, size, across


def kernel(
    nz, nt, lam_ref, q1_ref, q2_ref, gain_ref, k1_hbm, k2_hbm, v_hbm, res_hbm, ow_hbm, gate_hbm, up_hbm, down_hbm,
    out_ref,
    kv, gate, up, down, ow, res, qa, qb, m_ref, l_ref, acc_ref, att, mix_send, mix_recv, mix_own,
    stream, sq, xg, hid, ffn_send, ffn_recv, ffn_own,
    sent, zr, dr, yr, er, xs, xr, local,
):
    g, s, t = lax.axis_index("grp"), lax.axis_index("sp"), lax.axis_index("tp")
    z, c = s // 2, s % 2
    half = nz // 2
    rows = res.shape[0]
    pair = 2 * rows
    feat = res.shape[1]
    wrows = gate_hbm.shape[0]
    part = g % 2
    sign = 1 - 2 * c

    def wrap(v):
        return lax.rem(v + 2 * nz, nz)

    def chip(v):
        return (g, 2 * wrap(v) + c, t)

    partner = (g, s + sign, t)
    across = (g + 1 - 2 * part, s, t)

    def other(k):
        return lax.rem(t + k, nt)

    own_kv = pl.ds(pl.multiple_of(rows * s, 16), rows)
    own_w = pl.ds(pl.multiple_of(wrows * s, 16), wrows)
    k1_width, k2_width, v_width = k1_hbm.shape[1], k2_hbm.shape[1], v_hbm.shape[1]
    loads = [
        pltpu.make_async_copy(k1_hbm, kv.at[own_kv, pl.ds(0, k1_width)], local.at[0]),
        pltpu.make_async_copy(k2_hbm, kv.at[own_kv, pl.ds(k1_width, k2_width)], local.at[1]),
        pltpu.make_async_copy(v_hbm, kv.at[own_kv, pl.ds(k1_width + k2_width, v_width)], local.at[2]),
        pltpu.make_async_copy(up_hbm, up.at[own_w, :], local.at[3]),
        pltpu.make_async_copy(gate_hbm, gate.at[own_w, :], local.at[4]),
        pltpu.make_async_copy(down_hbm, down.at[own_w, :], local.at[5]),
        pltpu.make_async_copy(ow_hbm, ow, local.at[6]),
        pltpu.make_async_copy(res_hbm, res, local.at[7]),
    ]
    for load in loads:
        load.start()
    barrier = pltpu.get_barrier_semaphore()
    peers = [chip(z + 1), chip(z - 1), partner, across] + [(g, s, other(k)) for k in range(1, nt)]
    for peer in peers:
        pl.semaphore_signal(barrier, inc=1, device_id=peer, device_id_type=MESH)

    w1, w2 = q1_ref.shape[1], q2_ref.shape[1]
    lane1 = lax.broadcasted_iota(jnp.int32, (rows, w1), 1)
    lane2 = lax.broadcasted_iota(jnp.int32, (rows, w2), 1)
    q1, q2 = q1_ref[...], q2_ref[...]
    qa[pl.ds(0, rows), :] = jnp.where(lane1 < w1 // 2, q1, jnp.zeros_like(q1))
    qa[pl.ds(rows, rows), :] = jnp.where(lane1 < w1 // 2, jnp.zeros_like(q1), q1)
    qb[pl.ds(0, rows), :] = jnp.where(lane2 < w2 // 2, q2, jnp.zeros_like(q2))
    qb[pl.ds(rows, rows), :] = jnp.where(lane2 < w2 // 2, jnp.zeros_like(q2), q2)

    pl.semaphore_wait(barrier, len(peers))

    def view(ring, slot, start, size):
        return ring.buf.at[pl.ds(pl.multiple_of(ring.rows * slot + start, 8), size), :]

    def of_mine(ring, slot):
        shift = 0 if ring.across is None else ring.size * part
        return view(ring, slot, ring.low + shift, ring.size)

    def of_across(ring, slot):
        return view(ring, slot, ring.low + ring.size * (1 - part), ring.size)

    def remote(ring, ref, recv, device):
        return pltpu.make_async_remote_copy(
            src_ref=ref, dst_ref=ref, send_sem=sent.at[ring.index], recv_sem=recv,
            device_id=device, device_id_type=MESH,
        )

    def total(ring, count, recv):
        return remote(ring, ring.buf.at[pl.ds(0, count * ring.size), :], recv, partner)

    def at_distance(way, d):
        return 2 * (wrap(z - d) if way == 0 else wrap(z + d))

    def onward(ring, way, d):
        ref = of_mine(ring, at_distance(way, d) + c)
        return remote(ring, ref, zr.at[ring.index, way, d + 1], chip(z + 1 - 2 * way))

    def landed(ring, way, d):
        ref = of_mine(ring, at_distance(way, d) + c)
        remote(ring, ref, zr.at[ring.index, way, d], partner).wait_recv()

    def last_onward(ring):
        ref = of_mine(ring, 2 * wrap(z - (half - 1) * sign) + c)
        return remote(ring, ref, zr.at[ring.index, 0, half], chip(z + sign))

    def begin(rings):
        for ring in rings:
            for way in range(2):
                onward(ring, way, 0).start()
        for ring in rings:
            size = ring.size if ring.across is None else 2 * ring.size
            ref = view(ring, 2 * z + c, ring.low, size)
            remote(ring, ref, dr.at[ring.index, 0], partner).start()

    def pass_on(ring, way, d):
        ref = of_mine(ring, at_distance(way, d) + c)
        if ring.across is not None:
            remote(ring, ref, yr.at[ring.across, way, d], across).start()
        remote(ring, ref, dr.at[ring.index, d], partner).start()

    def take_across(ring, way, d):
        ref = of_across(ring, at_distance(way, d) + c)
        remote(ring, ref, yr.at[ring.across, way, d], across).wait_recv()
        remote(ring, ref, er.at[ring.across, d], partner).start()

    def from_partner(ring, d, count):
        if ring.across is not None:
            total(ring, 2 if count == 0 else count, dr.at[ring.index, d]).wait_recv()
            if count > 0:
                total(ring, count, er.at[ring.across, d]).wait_recv()
        else:
            total(ring, 1 if count == 0 else count, dr.at[ring.index, d]).wait_recv()

    def tick(rings, start, now):
        d = now - start
        if isinstance(start, int) and start > 0:

            @pl.when(d == 0)
            def _():
                begin(rings)

        @pl.when((d >= 1) & (d < half))
        def _():
            for ring in rings:
                for way in range(2):
                    landed(ring, way, d)

                    @pl.when(d < half - 1)
                    def _():
                        onward(ring, way, d).start()

                    pass_on(ring, way, d)

                    if ring.across is not None:

                        @pl.when(d > 1)
                        def _():
                            take_across(ring, way, d - 1)

            @pl.when(d == half - 1)
            def _():
                for ring in rings:
                    last_onward(ring).start()

        @pl.when(d == half)
        def _():
            for ring in rings:
                landed(ring, 0, half)
                pass_on(ring, 0, half)
                if ring.across is not None:
                    for way in range(2):
                        take_across(ring, way, half - 1)

        @pl.when(d == half + 1)
        def _():
            for ring in rings:
                if ring.across is not None:
                    take_across(ring, 0, half)

    def gather(rings, start, now):
        d = now - start

        @pl.when(d == 1)
        def _():
            for ring in rings:
                from_partner(ring, 0, 0)

        @pl.when((d > 1) & (d <= half))
        def _():
            for ring in rings:
                from_partner(ring, d - 1, 2)

        @pl.when(d == half + 1)
        def _():
            for ring in rings:
                from_partner(ring, half, 1)

    def all_sent(rings):
        for ring in rings:
            count = 4 * half - 1 if ring.across is None else 8 * half - 2
            total(ring, count, dr.at[ring.index, 0]).wait_send()

    cut = rows // 2
    kv_rings = [Ring(0, kv, rows, 0, cut), Ring(1, kv, rows, cut, cut)]
    up_rings = [Ring(2, up, wrows, 0, wrows // 2, across=0)]
    gate_rings = [
        Ring(3, gate, wrows, 0, SPLIT, across=1), Ring(4, gate, wrows, 2 * SPLIT, wrows - 2 * SPLIT)
    ]
    down_rings = [
        Ring(5, down, wrows, 0, SPLIT, across=2), Ring(6, down, wrows, 2 * SPLIT, wrows - 2 * SPLIT)
    ]

    value_size = acc_ref.shape[2]
    log2e = 1.4426950408889634
    k_cols = ((0, w1), (w1, w2))
    v_at = w1 + w2

    def attend(zk, first):
        at = pl.ds(pl.multiple_of(pair * zk, 16), pair)
        for group in range(2):
            q_ref = (qa, qb)[group]
            col, width = k_cols[group]
            factor = (width // 2) ** (-0.5) * log2e
            scores = lax.dot_general(
                q_ref[...], kv[at, pl.ds(col, width)], NT_DIMS, preferred_element_type=F32
            )
            if first:
                q_at = lax.broadcasted_iota(jnp.int32, (pair, pair), 0)
                k_at = lax.broadcasted_iota(jnp.int32, (pair, pair), 1)
                q_at = jnp.where(q_at >= rows, q_at - rows, q_at) + rows * c
                scores = jnp.where(k_at <= q_at, scores, -1e30)
            peak = jnp.max(scores, axis=1, keepdims=True)
            if not first:
                old = m_ref[group][:, :1]
                peak = jnp.maximum(old, peak)
                alpha = jnp.exp2((old - peak) * factor)
            weights = jnp.exp2((scores - peak) * factor)
            total = jnp.sum(weights, axis=1, keepdims=True)
            values = kv[at, pl.ds(v_at + group * value_size, value_size)]
            out = jnp.dot(weights.astype(BF16), values, preferred_element_type=F32)
            if not first:
                total = total + alpha * l_ref[group][:, :1]
                out = out + alpha * acc_ref[group]
            m_ref[group] = jnp.broadcast_to(peak, (pair, 128))
            l_ref[group] = jnp.broadcast_to(total, (pair, 128))
            acc_ref[group] = out

    def attend_step(d):
        def one(i, carry):
            zk = jnp.where(i == 0, z - d, z + d - nz)

            @pl.when(zk >= 0)
            def _():
                attend(zk, False)

            return carry

        lax.fori_loop(0, 2, one, 0)

    def swap(ref_from, ref_to, which, k):
        return pltpu.make_async_remote_copy(
            src_ref=ref_from, dst_ref=ref_to, send_sem=xs.at[which, k - 1], recv_sem=xr.at[which, k - 1],
            device_id=(g, s, other(k)), device_id_type=MESH,
        )

    def mine(which, k):
        if which == 0:
            return swap(mix_send.at[k - 1], mix_recv.at[k - 1], 0, k)
        if which == 1:
            cols = xg.at[:, pl.ds(pl.multiple_of(feat * t, 128), feat)]
            return swap(cols, cols, 1, k)
        if which == 2:
            return swap(sq.at[t], sq.at[t], 2, k)
        return swap(ffn_send.at[k - 1], ffn_recv.at[k - 1], 3, k)

    def theirs(which, k):
        frm = lax.rem(t + nt - k, nt)
        if which == 1:
            cols = xg.at[:, pl.ds(pl.multiple_of(feat * frm, 128), feat)]
            return swap(cols, cols, 1, k)
        if which == 2:
            return swap(sq.at[frm], sq.at[frm], 2, k)
        return mine(which, k)

    for load in loads[:3]:
        load.wait()
    begin(kv_rings)
    loads[3].wait()
    begin(up_rings)
    for load in loads[4:6]:
        load.wait()

    def project():
        for group in range(2):
            map_out = acc_ref[group] / l_ref[group]
            differ = map_out[:rows] - lam_ref[0, group] * map_out[rows:]
            scale = lax.rsqrt(jnp.mean(differ * differ, axis=1, keepdims=True) + 1e-06)
            att[:, pl.ds(group * value_size, value_size)] = (0.8 * differ * scale).astype(BF16)
        loads[6].wait()
        for k in ORDER:
            cols = pl.ds(pl.multiple_of(feat * other(k), 128), feat)
            mix_send[k - 1] = jnp.dot(att[...], ow[:, cols], preferred_element_type=F32).astype(BF16)
        mix_own[...] = jnp.dot(
            att[...], ow[:, pl.ds(pl.multiple_of(feat * t, 128), feat)], preferred_element_type=F32
        )
        for k in ORDER:
            mine(0, k).start()
        loads[7].wait()

    def make_stream():
        acc = mix_own[...] + res[...].astype(F32)
        for k in ORDER:
            theirs(0, k).wait_recv()
            acc = acc + mix_recv[k - 1].astype(F32)
        stream[...] = acc
        sq[t] = jnp.broadcast_to(jnp.sum(acc * acc, axis=1, keepdims=True), sq.shape[1:])
        xg[:, pl.ds(pl.multiple_of(feat * t, 128), feat)] = (acc * gain_ref[...].astype(F32)).astype(BF16)
        for k in ORDER:
            mine(1, k).start()
            mine(2, k).start()

    hidden = hid.shape[1]
    tile = 256
    tiles, rest = hidden // tile, hidden % tile

    def hidden_tile(cols):
        scale = m_ref[0, pl.ds(0, rows), :][:, :1]
        gates = jnp.dot(xg[...], gate[:, cols], preferred_element_type=F32) * scale
        ups = jnp.dot(xg[...], up[:, cols], preferred_element_type=F32) * scale
        hid[:, cols] = (gates / (1.0 + jnp.exp(-gates)) * ups).astype(BF16)

    def hidden_units():
        for k in ORDER:
            theirs(1, k).wait_recv()
            theirs(2, k).wait_recv()
        squares = sq[0]
        for k in range(1, nt):
            squares = squares + sq[k]
        m_ref[0, pl.ds(0, rows), :] = lax.rsqrt(squares / (feat * nt) + 1e-06)

        def one(i, carry):
            hidden_tile(pl.ds(pl.multiple_of(i * tile, 128), tile))
            return carry

        lax.fori_loop(0, tiles, one, 0)
        hidden_tile(pl.ds(tiles * tile, rest))

    def give(zz):
        width = 2 * wrows
        owner = zz // (nz // nt)
        cols = pl.ds(pl.multiple_of(width * lax.rem(zz, nz // nt), 128), width)
        value = lax.dot_general(
            hid[...], down[pl.ds(pl.multiple_of(width * zz, 16), width), :], NT_DIMS,
            preferred_element_type=F32,
        )
        k = lax.rem(owner - t + nt, nt)

        @pl.when(k == 0)
        def _():
            ffn_own[:, cols] = value

        @pl.when(k > 0)
        def _():
            ffn_send[k - 1, :, cols] = value.astype(BF16)
            swap(ffn_send.at[k - 1, :, cols], ffn_recv.at[k - 1, :, cols], 3, k).start()

    def give_both(d):
        def one(i, carry):
            give(wrap(jnp.where(i == 0, z - d, z + d)))
            return carry

        lax.fori_loop(0, 2, one, 0)

    last = DOWN_AT + half + 1

    def all_steps(now, carry):
        tick(kv_rings, 0, now)
        tick(up_rings, 0, now)
        tick(gate_rings, GATE_AT, now)
        tick(down_rings, DOWN_AT, now)

        gather(kv_rings, 0, now)

        @pl.when(now == 1)
        def _():
            attend(z, True)

        @pl.when((now > 1) & (now <= half))
        def _():
            attend_step(now - 1)

        @pl.when(now == half + 1)
        def _():
            @pl.when(z >= half)
            def _():
                attend(z - half, False)

            project()

        @pl.when(now == STREAM_AT)
        def _():
            make_stream()

        gather(up_rings, 1, now)
        gather(gate_rings, GATE_AT, now)
        gather(down_rings, DOWN_AT, now)

        @pl.when(now == HIDDEN_AT)
        def _():
            hidden_units()
            give(z)

            def one(d, carry):
                give_both(d)
                return carry

            lax.fori_loop(1, HIDDEN_AT - DOWN_AT, one, 0)

        @pl.when((now > HIDDEN_AT) & (now < last))
        def _():
            give_both(now - 1 - DOWN_AT)

        @pl.when(now == last)
        def _():
            give(wrap(z + half))

        return carry

    lax.fori_loop(1, last + 1, all_steps, 0)
    all_sent(kv_rings + up_rings + gate_rings + down_rings)
    for which in range(3):
        for k in range(1, nt):
            mine(which, k).wait_send()
    acc = ffn_own[...]
    for k in range(1, nt):
        theirs(3, k).wait_recv()
        acc = acc + ffn_recv[k - 1].astype(F32)
    out_ref[...] = (stream[...] + 0.5 * acc).astype(BF16)
    for k in range(1, nt):
        mine(3, k).wait_send()


def layer(
    nz, nt, query_first, key_first, query_second, key_second, values, lambdas, residual, norm_gain,
    out_weight, gate_weight, up_weight, down_weight,
):
    rows, feat = residual.shape
    wrows, hidden = gate_weight.shape
    value_size = values.shape[2]
    model = feat * nt
    kv_width = key_first.shape[1] + key_second.shape[1] + 2 * value_size
    w1, w2 = query_first.shape[1], query_second.shape[1]
    any_ref = pl.BlockSpec(memory_space=pltpu.HBM)
    vmem = pl.BlockSpec(memory_space=pltpu.VMEM)
    half = nz // 2
    dma = pltpu.SemaphoreType.DMA
    return pl.pallas_call(
        functools.partial(kernel, nz, nt),
        out_shape=jax.ShapeDtypeStruct((rows, feat), BF16),
        in_specs=[pl.BlockSpec(memory_space=pltpu.SMEM), vmem, vmem, vmem] + [any_ref] * 8,
        out_specs=vmem,
        scratch_shapes=[
            pltpu.VMEM((2 * nz * rows, kv_width), BF16),
            pltpu.VMEM((2 * nz * wrows, hidden), BF16),
            pltpu.VMEM((2 * nz * wrows, hidden), BF16),
            pltpu.VMEM((2 * nz * wrows, hidden), BF16),
            pltpu.VMEM((2 * value_size, model), BF16),
            pltpu.VMEM((rows, feat), BF16),
            pltpu.VMEM((2 * rows, w1), BF16),
            pltpu.VMEM((2 * rows, w2), BF16),
            pltpu.VMEM((2, 2 * rows, 128), F32),
            pltpu.VMEM((2, 2 * rows, 128), F32),
            pltpu.VMEM((2, 2 * rows, value_size), F32),
            pltpu.VMEM((rows, 2 * value_size), BF16),
            pltpu.VMEM((nt - 1, rows, feat), BF16),
            pltpu.VMEM((nt - 1, rows, feat), BF16),
            pltpu.VMEM((rows, feat), F32),
            pltpu.VMEM((rows, feat), F32),
            pltpu.VMEM((nt, rows, 128), F32),
            pltpu.VMEM((rows, model), BF16),
            pltpu.VMEM((rows, hidden), BF16),
            pltpu.VMEM((nt - 1, rows, feat), BF16),
            pltpu.VMEM((nt - 1, rows, feat), BF16),
            pltpu.VMEM((rows, feat), F32),
            dma((7,)),
            dma((7, 2, half + 1)),
            dma((7, half + 1)),
            dma((3, 2, half + 1)),
            dma((3, half + 1)),
            dma((4, nt - 1)),
            dma((4, nt - 1)),
            dma((8,)),
        ],
        compiler_params=pltpu.CompilerParams(
            collective_id=0, has_side_effects=True, vmem_limit_bytes=60 * 2**20
        ),
    )(
        lambdas.T, query_first, query_second, norm_gain.reshape(1, feat), key_first, key_second,
        values.reshape(rows, -1), residual,
        out_weight.reshape(2 * value_size, model), gate_weight, up_weight, down_weight.T,
    )


def solution(mesh):
    return jax.shard_map(
        functools.partial(layer, mesh.shape["sp"] // 2, mesh.shape["tp"]),
        mesh=mesh,
        in_specs=(
            P(("grp", "sp"), "tp"),
            P(("grp", "sp"), "tp"),
            P(("grp", "sp"), "tp"),
            P(("grp", "sp"), "tp"),
            P(("grp", "sp"), None, "tp"),
            P(None, "tp"),
            P(("grp", "sp"), "tp"),
            P("tp"),
            P(None, "tp", None),
            P("sp", "tp"),
            P("sp", "tp"),
            P("tp", "sp"),
        ),
        out_specs=P(("grp", "sp"), "tp"),
        check_vma=False,
    )
```
